32 devices in a mesh: sp: 8 (over z, y), tp: 4 (over x, core).
Axes of the slice: x: 2, y: 2, z: 4, core: 2. Of those that a mesh axis runs over, the one named last changes fastest.
Arguments:
- tokens: bfloat16 [4096, 2048], P('sp', 'tp'), may hold values from -6 to 6
- in_gain: float32 [2048], replicated, may hold values from 0.1 to 1.9
- conv_value_w: bfloat16 [2048, 1024], P(None, 'tp'), may hold values from -0.125 to 0.125
- conv_gate_w: bfloat16 [2048, 1024], P(None, 'tp'), may hold values from -0.125 to 0.125
- conv_taps: float32 [31, 1024], P(None, 'tp'), may hold values from -8 to 8
- conv_gain: float32 [1024], P('tp'), may hold values from 0.1 to 1.9
- query_latent_weight: bfloat16 [2048, 512], replicated, may hold values from -0.125 to 0.125
- latent_weight: bfloat16 [2048, 512], replicated, may hold values from -0.125 to 0.125
- rope_key_w: bfloat16 [2048, 64], replicated, may hold values from -0.125 to 0.125
- query_gain: float32 [512], replicated, may hold values from 1.5 to 8, as said below
- latent_gain: float32 [512], replicated, may hold values from 1.5 to 8, as said below
- query_weight: bfloat16 [512, 1024], P(None, 'tp'), may hold values from -0.25 to 0.25
- query_rotary_weight: bfloat16 [512, 512], P(None, 'tp'), may hold values from -0.25 to 0.25
- key_weight: bfloat16 [512, 1024], P(None, 'tp'), may hold values from -0.25 to 0.25
- value_weight: bfloat16 [512, 1024], P(None, 'tp'), may hold values from -0.25 to 0.25
- conv_out_w: bfloat16 [1024, 2048], P('tp'), may hold values from -0.125 to 0.125
- attn_out_w: bfloat16 [1024, 2048], P('tp'), may hold values from -0.125 to 0.125
- out_gain: float32 [2048], replicated, may hold values from 0.1 to 1.9
Outputs:
- mixed: bfloat16 [4096, 2048], P(('sp', 'tp'))
The draws below stay inside these ranges and needn't reach their ends.
Inputs may be any that keep to these rules, and one draw needn't show every extreme that they name: `query_gain`: positive gains. `latent_gain`: positive gains.
All inputs are finite; a program needn't handle non-finite values.
Results may differ from the reference program's by a relative error of at most 0.018.
The reference program's roundings to bfloat16 on the way count: a program that leaves them out, or rounds other values in their place, can miss the bound.
Values may be sent and summed in bfloat16 or wider, within the bound.
A program may use at most 128 MiB of HBM per device.

```python
import math
import jax
import jax.numpy as jnp
from jax import lax

MODEL_WIDTH = 2048
CONV_CH = 1024
CONV_K = 31
HALF_K = 15
HEAD_COUNT = 8
HEAD_WIDTH = 128
ROTARY_WIDTH = 64
QUERY_LATENT = 512
LATENT_WIDTH = 512
TOKENS = 4096
N_TP = 4


def draw_conv_taps(key, part):
    first_key, second_key = jax.random.split(jax.random.fold_in(key, 11))
    channel_place = jnp.arange(CONV_CH, dtype=jnp.float32) / CONV_CH
    jitter = jax.random.uniform(first_key, (CONV_CH,), jnp.float32)
    exponent = 0.5 * channel_place + 0.5 * jitter
    base = jnp.clip(jax.random.normal(second_key, (CONV_K, CONV_CH), jnp.float32), -4.0, 4.0)
    return base * CONV_K ** (-0.5) * (10.0 ** exponent)[None, :]


def draw_gain_vector(key, width):
    jitter = jax.random.uniform(key, (width,), jnp.float32)
    lower, upper = (1.5, 3.0)
    return jnp.exp(jnp.log(lower) + jitter * (jnp.log(upper) - jnp.log(lower)))


def draw_query_gain(key, part):
    return draw_gain_vector(jax.random.fold_in(key, 23), QUERY_LATENT)


def draw_latent_gain(key, part):
    return draw_gain_vector(jax.random.fold_in(key, 37), LATENT_WIDTH)


def block_levels(own_key, dims, cuts, low, high):
    loudness = 1.0
    for position, shards_of in cuts:
        draws = jax.random.uniform(jax.random.fold_in(jax.random.fold_in(own_key, 6), position), (shards_of,), jnp.float32, low / len(cuts), high / len(cuts))
        loudness = loudness * jnp.repeat(jnp.exp(draws), dims[position] // shards_of).reshape((-1,) + (1,) * (len(dims) - 1 - position))
    return loudness


def bell_draw(rng, shape, spread, reach, shards=(), held_as=jnp.bfloat16):
    entries = spread * jax.random.normal(rng, shape, jnp.float32)
    if shards:
        entries = entries * block_levels(rng, shape, shards, -0.22, 0.18)
    return jnp.clip(entries, -reach, reach).astype(held_as)


def setup_inputs(seed: int = 0) -> dict:
    splits = jax.random.split(jax.random.key(seed), 19)
    tokens = bell_draw(splits[0], (TOKENS, MODEL_WIDTH), 1.0, 6.0, ((0, 8), (1, 4)))
    in_gain = jnp.clip(1.0 + 0.18 * jax.random.normal(splits[1], (MODEL_WIDTH,), jnp.float32), 0.1, 1.9)
    conv_value_w = bell_draw(splits[2], (MODEL_WIDTH, CONV_CH), MODEL_WIDTH ** -0.5, 0.125, ((1, 4),))
    conv_gate_w = bell_draw(splits[3], (MODEL_WIDTH, CONV_CH), MODEL_WIDTH ** -0.5, 0.125, ((1, 4),))
    conv_taps = draw_conv_taps(jax.random.fold_in(splits[18], 71), 0)
    conv_gain = jnp.clip(1.0 + 0.18 * jax.random.normal(splits[5], (CONV_CH,), jnp.float32), 0.1, 1.9)
    query_latent_weight = bell_draw(splits[6], (MODEL_WIDTH, QUERY_LATENT), MODEL_WIDTH ** -0.5, 0.125)
    latent_weight = bell_draw(splits[7], (MODEL_WIDTH, LATENT_WIDTH), MODEL_WIDTH ** -0.5, 0.125)
    rope_key_w = bell_draw(splits[8], (MODEL_WIDTH, ROTARY_WIDTH), MODEL_WIDTH ** -0.5, 0.125)
    query_gain = draw_query_gain(jax.random.fold_in(splits[18], 71), 0)
    latent_gain = draw_latent_gain(jax.random.fold_in(splits[18], 71), 0)
    query_weight = bell_draw(splits[11], (QUERY_LATENT, HEAD_COUNT * HEAD_WIDTH), QUERY_LATENT ** -0.5, 0.25, ((1, 4),))
    query_rotary_weight = bell_draw(splits[12], (QUERY_LATENT, HEAD_COUNT * ROTARY_WIDTH), QUERY_LATENT ** -0.5, 0.25, ((1, 4),))
    key_weight = bell_draw(splits[13], (LATENT_WIDTH, HEAD_COUNT * HEAD_WIDTH), LATENT_WIDTH ** -0.5, 0.25, ((1, 4),))
    value_weight = bell_draw(splits[14], (LATENT_WIDTH, HEAD_COUNT * HEAD_WIDTH), LATENT_WIDTH ** -0.5, 0.25, ((1, 4),))
    conv_out_w = bell_draw(splits[15], (CONV_CH, MODEL_WIDTH), (CONV_CH + HEAD_COUNT * HEAD_WIDTH) ** -0.5, 0.125, ((0, 4),))
    attn_out_w = bell_draw(splits[16], (HEAD_COUNT * HEAD_WIDTH, MODEL_WIDTH), (CONV_CH + HEAD_COUNT * HEAD_WIDTH) ** -0.5, 0.125, ((0, 4),))
    out_gain = jnp.clip(1.0 + 0.18 * jax.random.normal(splits[17], (MODEL_WIDTH,), jnp.float32), 0.1, 1.9)
    return {"tokens": tokens, "in_gain": in_gain, "conv_value_w": conv_value_w, "conv_gate_w": conv_gate_w, "conv_taps": conv_taps, "conv_gain": conv_gain, "query_latent_weight": query_latent_weight, "latent_weight": latent_weight, "rope_key_w": rope_key_w, "query_gain": query_gain, "latent_gain": latent_gain, "query_weight": query_weight, "query_rotary_weight": query_rotary_weight, "key_weight": key_weight, "value_weight": value_weight, "conv_out_w": conv_out_w, "attn_out_w": attn_out_w, "out_gain": out_gain}


norm_eps = 1e-06
layer_eps = 1e-05
rope_base = 10000.0

def to_float(values):
    return lax.optimization_barrier(values).astype(jnp.float32)

def rms_scaled(values, gain):
    return values * lax.rsqrt(lax.optimization_barrier(jnp.mean(values * values, axis=-1, keepdims=True)) + norm_eps) * gain

def rotate(values, cosine_table, sine_table):
    halfway = values.shape[-1] // 2
    first = values[..., :halfway]
    second = values[..., halfway:]
    return jnp.concatenate([first * cosine_table - second * sine_table, second * cosine_table + first * sine_table], axis=-1)

def tables(positions, width):
    halfway = width // 2
    inverse = rope_base ** (-jnp.arange(halfway, dtype=jnp.float32) / halfway)
    angles = positions[:, None] * inverse[None, :]
    return (jnp.cos(angles), jnp.sin(angles))

def reference(tokens, in_gain, conv_value_w, conv_gate_w, conv_taps, conv_gain, query_latent_weight, latent_weight, rope_key_w, query_gain, latent_gain, query_weight, query_rotary_weight, key_weight, value_weight, conv_out_w, attn_out_w, out_gain):
    tokens_all = tokens.shape[0]
    normed = rms_scaled(tokens.astype(jnp.float32), in_gain).astype(jnp.bfloat16)
    conv_value = jnp.dot(normed, conv_value_w, preferred_element_type=jnp.float32)
    conv_gate = jnp.dot(normed, conv_gate_w, preferred_element_type=jnp.float32)
    gated = (conv_value * jax.nn.sigmoid(conv_gate)).astype(jnp.bfloat16)
    padded = jnp.pad(to_float(gated), ((HALF_K, HALF_K), (0, 0)))
    convolved = jnp.zeros((tokens_all, CONV_CH), jnp.float32)
    for offset_tap in range(CONV_K):
        convolved = convolved + conv_taps[offset_tap] * padded[offset_tap:offset_tap + tokens_all]
    chan_mean = lax.optimization_barrier(jnp.mean(convolved, axis=1, keepdims=True))
    chan_square = lax.optimization_barrier(jnp.mean(convolved * convolved, axis=1, keepdims=True))
    shaped = (convolved - chan_mean) * lax.rsqrt(chan_square - chan_mean * chan_mean + layer_eps) * conv_gain
    conv_result = jax.nn.silu(shaped).astype(jnp.bfloat16)
    positions = jnp.arange(tokens_all, dtype=jnp.int32).astype(jnp.float32)
    cosine_table, sine_table = tables(positions, ROTARY_WIDTH)
    query_lat = rms_scaled(jnp.dot(normed, query_latent_weight, preferred_element_type=jnp.float32), query_gain).astype(jnp.bfloat16)
    latent = rms_scaled(jnp.dot(normed, latent_weight, preferred_element_type=jnp.float32), latent_gain).astype(jnp.bfloat16)
    rope_keys = rotate(jnp.dot(normed, rope_key_w, preferred_element_type=jnp.float32), cosine_table, sine_table).astype(jnp.bfloat16)
    query_main = jnp.dot(query_lat, query_weight, preferred_element_type=jnp.float32).astype(jnp.bfloat16).reshape(tokens_all, HEAD_COUNT, HEAD_WIDTH)
    query_rope = rotate(jnp.dot(query_lat, query_rotary_weight, preferred_element_type=jnp.float32).reshape(tokens_all, HEAD_COUNT, ROTARY_WIDTH), cosine_table[:, None, :], sine_table[:, None, :]).astype(jnp.bfloat16)
    key_float = to_float(jnp.dot(latent, key_weight, preferred_element_type=jnp.float32).astype(jnp.bfloat16)).reshape(tokens_all, HEAD_COUNT, HEAD_WIDTH)
    value_float = to_float(jnp.dot(latent, value_weight, preferred_element_type=jnp.float32).astype(jnp.bfloat16)).reshape(tokens_all, HEAD_COUNT, HEAD_WIDTH)
    rope_float = to_float(rope_keys)
    score_scale = (HEAD_WIDTH + ROTARY_WIDTH) ** (-0.5)
    query_block = math.gcd(tokens_all, 512)
    block_count = tokens_all // query_block

    def one_block(pieces):
        block_main, block_rope = pieces
        scores = (jnp.einsum('thd,khd->htk', to_float(block_main), key_float) + jnp.einsum('thr,kr->htk', to_float(block_rope), rope_float)) * score_scale
        top_score = lax.optimization_barrier(jnp.max(scores, axis=-1, keepdims=True))
        weights = jnp.exp(scores - top_score)
        totals = lax.optimization_barrier(jnp.sum(weights, axis=-1))
        summed = jnp.einsum('htk,khd->thd', to_float(weights.astype(jnp.bfloat16)), value_float)
        return (summed / totals.T[:, :, None]).astype(jnp.bfloat16)
    blocks_out = lax.map(one_block, (query_main.reshape(block_count, query_block, HEAD_COUNT, HEAD_WIDTH), query_rope.reshape(block_count, query_block, HEAD_COUNT, ROTARY_WIDTH)))
    attention_result = blocks_out.reshape(tokens_all, HEAD_COUNT * HEAD_WIDTH)
    chan_share = CONV_CH // N_TP
    head_share = HEAD_COUNT * HEAD_WIDTH // N_TP
    merged = jnp.zeros((tokens_all, MODEL_WIDTH), jnp.float32)
    for group in range(N_TP):
        partial_value = jnp.dot(conv_result[:, group * chan_share:(group + 1) * chan_share], conv_out_w[group * chan_share:(group + 1) * chan_share], preferred_element_type=jnp.float32) + jnp.dot(attention_result[:, group * head_share:(group + 1) * head_share], attn_out_w[group * head_share:(group + 1) * head_share], preferred_element_type=jnp.float32)
        merged = merged + to_float(partial_value.astype(jnp.bfloat16))
    return rms_scaled(merged, out_gain).astype(jnp.bfloat16)
```

```python
import functools

import jax
import jax.numpy as jnp
from jax import lax
from jax.experimental import pallas as pl
from jax.experimental.pallas import tpu as pltpu
from jax.sharding import PartitionSpec as P

HEAD_WIDTH = 128
norm_eps = 1e-06
layer_eps = 1e-05
rope_base = 10000.0
CHUNKS = 4
MESH = pl.DeviceIdType.MESH
F32 = jnp.float32
BF16 = jnp.bfloat16


def dot(a, b):
    return jnp.dot(a, b, preferred_element_type=F32)


def dot_nt(a, b):
    return lax.dot_general(a, b, (((1,), (1,)), ((), ())), preferred_element_type=F32)


def rms(values, gain):
    return values * lax.rsqrt(jnp.mean(values * values, axis=-1, keepdims=True) + norm_eps) * gain


def rotate_pair(values, cosine, sine):
    lane = lax.broadcasted_iota(jnp.int32, values.shape, 1)
    swapped = jnp.where(
        lane % 64 < 32, pltpu.roll(values, 96, 1), pltpu.roll(values, 32, 1)
    )
    return values * cosine + swapped * sine


def layer(
    cfg,
    tokens, in_gain, cvw, cgw, taps, conv_gain, qlw, lw, rkw, q_gain, l_gain,
    qw, qrw, kw, vw, cow, aow, out_gain, cosine, sine,
    out,
    xb, v_cvw, v_cgw, v_qlw, v_lw, v_rkw, v_qw, v_qrw, v_kw, v_vw, v_cow, v_aow,
    nb, kvb, halo_s, halo_r, pad, conv, st_col, st_s, st_r, crs, qs, mx, acc, ars,
    psb, pr, pa, xr,
    tok_sem, w_sem, xs_send, xs_fwd, xs_recv, g_recv, g_zs, g_ys, g_ps,
    h_send, h_recv, t_send, t_recv, p_send, p_recv, r_send, r_recv,
):
    S, TP, Z, Y, X, T, F, D, C, H = cfg
    R = T // CHUNKS
    Tb = T // TP
    s = lax.axis_index("sp")
    t = lax.axis_index("tp")
    z, y = s // Y, s % Y
    x, c = t // 2, t % 2
    mate = x * 2 + (1 - c)

    def remote(src, dst, ss, rs, dev):
        return pltpu.make_async_remote_copy(
            src_ref=src, dst_ref=dst, send_sem=ss, recv_sem=rs, device_id=dev, device_id_type=MESH
        )

    tok_copies = [
        pltpu.make_async_copy(
            tokens.at[pl.ds(r * R, R), :], xb.at[t, pl.ds(r * R, R), :], tok_sem.at[r]
        )
        for r in range(CHUNKS)
    ]
    pairs = [
        (lw, v_lw), (rkw, v_rkw), (cvw, v_cvw), (cgw, v_cgw), (qlw, v_qlw), (qw, v_qw),
        (qrw, v_qrw), (kw, v_kw), (vw, v_vw), (cow, v_cow), (aow, v_aow),
    ]
    w_copies = [pltpu.make_async_copy(a, b, w_sem.at[i]) for i, (a, b) in enumerate(pairs)]
    for cp in tok_copies + w_copies:
        cp.start()

    barrier = pltpu.get_barrier_semaphore()
    peers = [(s, (t + e) % TP) for e in range(1, TP)]
    peers += [(((z + e) % Z) * Y + y, t) for e in (1, Z - 1)]
    peers += [(z * Y + (y + e) % Y, t) for e in range(1, Y)]
    peers += [((s + e) % S, t) for e in (1, S - 1)]
    for dev in peers:
        pl.semaphore_signal(barrier, inc=1, device_id=dev, device_id_type=MESH)
    pl.semaphore_wait(barrier, len(peers))

    def tok_copy(src, r, ss, dev):
        blk = xb.at[src, pl.ds(r * R, R), :]
        return remote(blk, blk, ss, xs_recv.at[src, r], dev)

    own_sends = []
    for r in range(CHUNKS):
        tok_copies[r].wait()
        for e in range(1, X):
            cp = tok_copy(t, r, xs_send.at[e, r], (s, ((x + e) % X) * 2 + c))
            cp.start()
            own_sends.append(cp)
        cp = tok_copy(t, r, xs_send.at[0, r], (s, mate))
        cp.start()
        own_sends.append(cp)

    def slot(src, r):
        return kvb.at[src, r]

    def z_copy(zs, i, up):
        src, r = zs * Y + y, c + 2 * i
        step = 1 if up else -1
        return remote(
            slot(src, r), slot(src, r), g_zs.at[0 if up else 1, zs, i], g_recv.at[src, r],
            ((z + step) * Y + y, t),
        )

    def y_copy(zs, i, e):
        src, r = zs * Y + y, c + 2 * i
        return remote(
            slot(src, r), slot(src, r), g_ys.at[e - 1, zs, i], g_recv.at[src, r],
            (z * Y + (y + e) % Y, t),
        )

    def mate_copy(src, i):
        r = c + 2 * i
        return remote(
            slot(src, r), slot(src, r), g_ps.at[src, i], g_recv.at[src, r], (s, mate)
        )

    def arrived(src, r):
        remote(
            slot(src, r), slot(src, r), g_ps.at[src, 0], g_recv.at[src, r], (s, mate)
        ).wait_recv()

    def relay(d, i):
        lo, hi = z - d, z + d

        @pl.when(lo >= 0)
        def _():
            arrived(lo * Y + y, c + 2 * i)

            @pl.when(z + 1 < Z)
            def _():
                z_copy(lo, i, True).start()

            for e in range(1, Y):
                y_copy(lo, i, e).start()
            mate_copy(lo * Y + y, i).start()

        @pl.when(hi < Z)
        def _():
            arrived(hi * Y + y, c + 2 * i)

            @pl.when(z - 1 >= 0)
            def _():
                z_copy(hi, i, False).start()

            for e in range(1, Y):
                y_copy(hi, i, e).start()
            mate_copy(hi * Y + y, i).start()

    fwd_sends = []
    lane = lax.broadcasted_iota(jnp.int32, (R // 8, 128), 1)
    for r in range(CHUNKS):
        rows = pl.ds(r * R, R)
        for e in range(1, X):
            src = ((x + e) % X) * 2 + c
            tok_copy(src, r, xs_send.at[e, r], (s, mate)).wait_recv()
            cp = tok_copy(src, r, xs_fwd.at[e - 1, r], (s, mate))
            cp.start()
            fwd_sends.append(cp)
        for e in range(X):
            src = ((x + e) % X) * 2 + (1 - c)
            tok_copy(src, r, xs_send.at[0, r], (s, mate)).wait_recv()
        total = jnp.zeros((R, 1), F32)
        for g in range(TP):
            v = xb[g, rows, :].astype(F32)
            total += jnp.sum(v * v, axis=1, keepdims=True)
        scale = lax.rsqrt(total / D + norm_eps)
        for g in range(TP):
            cols = slice(g * F, (g + 1) * F)
            nb[rows, cols] = (xb[g, rows, :].astype(F32) * scale * in_gain[:, cols]).astype(BF16)
        if r == 0:
            w_copies[0].wait()
            w_copies[1].wait()
        n = nb[rows, :]
        kvb[s, r, 0:R, :] = rms(dot(n, v_lw[...]), l_gain[...]).astype(BF16)
        rk = rotate_pair(dot(n, v_rkw[...]), cosine[rows, :], sine[rows, :])
        per = R // 8
        for k in range(4):
            kvb[s, r, R : R + per, 128 * k : 128 * (k + 1)] = jnp.where(
                lane < 64, rk[2 * per * k : 2 * per * k + per], rk[2 * per * k + per : 2 * per * (k + 1)]
            ).astype(BF16)

        @pl.when(c == r % 2)
        def _():
            i = r // 2
            src = z * Y + y

            @pl.when(z + 1 < Z)
            def _():
                z_copy(z, i, True).start()

            @pl.when(z - 1 >= 0)
            def _():
                z_copy(z, i, False).start()

            for e in range(1, Y):
                y_copy(z, i, e).start()

        if r == 2:
            relay(1, 0)

    for k in (2, 3):
        w_copies[k].wait()
    for q in range(2):
        rows = pl.ds(q * (T // 2), T // 2)
        n = nb[rows, :]
        cv = dot(n, v_cvw[...])
        cg = dot(n, v_cgw[...])
        gated = (cv * jax.nn.sigmoid(cg)).astype(BF16)
        if q == 0:
            halo_s[0] = gated[0:16]
        else:
            halo_s[1] = gated[T // 2 - 16 :]
        gf = gated.astype(F32)
        for l in range(C // 128):
            pad[l, 16 + q * (T // 2) : 16 + (q + 1) * (T // 2), :] = gf[:, 128 * l : 128 * (l + 1)]

    def halo(up):
        k = 1 if up else 0
        return remote(
            halo_s.at[k], halo_r.at[1 - k], h_send.at[k], h_recv.at[1 - k],
            (s + 1 if up else s - 1, t),
        )

    @pl.when(s > 0)
    def _():
        halo(False).start()

    @pl.when(s < S - 1)
    def _():
        halo(True).start()

    relay(1, 1)

    for k in (4, 5, 6):
        w_copies[k].wait()
    for q in range(2):
        rows = pl.ds(q * (T // 2), T // 2)
        ql = rms(dot(nb[rows, :], v_qlw[...]), q_gain[...]).astype(BF16)
        qm = dot(ql, v_qw[...])
        qr = dot(ql, v_qrw[...])
        half = lax.broadcasted_iota(jnp.int32, (T // 2, 128), 1) < 64
        for h in range(H):
            hs = slice(128 * h, 128 * (h + 1))
            qs[h, rows, 0:128] = qm[:, hs].astype(BF16)
            rot = rotate_pair(qr[:, hs], cosine[rows, :], sine[rows, :])
            qs[h, rows, 128:256] = jnp.where(half, rot, 0.0).astype(BF16)

    relay(2, 0)

    @pl.when(s > 0)
    def _():
        remote(halo_s.at[1], halo_r.at[0], h_send.at[1], h_recv.at[0], (s - 1, t)).wait_recv()
        for l in range(C // 128):
            pad[l, 0:16, :] = halo_r[0, :, 128 * l : 128 * (l + 1)].astype(F32)

    @pl.when(s == 0)
    def _():
        for l in range(C // 128):
            pad[l, 0:16, :] = jnp.zeros((16, 128), F32)

    @pl.when(s < S - 1)
    def _():
        remote(halo_s.at[0], halo_r.at[1], h_send.at[0], h_recv.at[1], (s + 1, t)).wait_recv()
        for l in range(C // 128):
            pad[l, T + 16 : T + 32, :] = halo_r[1, :, 128 * l : 128 * (l + 1)].astype(F32)

    @pl.when(s == S - 1)
    def _():
        for l in range(C // 128):
            pad[l, T + 16 : T + 32, :] = jnp.zeros((16, 128), F32)

    K = taps.shape[0]
    B = 64

    def conv_tile(i, carry):
        base = i * B
        s1 = jnp.zeros((B, 128), F32)
        s2 = jnp.zeros((B, 128), F32)
        for l in range(C // 128):
            a = jnp.zeros((B, 128), F32)
            for j in range(K):
                off = 16 - K // 2 + j
                a += taps[j : j + 1, 128 * l : 128 * (l + 1)] * pad[l, pl.ds(base + off, B), :]
            conv[pl.ds(pl.multiple_of(base, B), B), 128 * l : 128 * (l + 1)] = a
            s1 += a
            s2 += a * a
        lanes = lax.broadcasted_iota(jnp.int32, (B, 128), 1)
        r1 = jnp.sum(s1, axis=1, keepdims=True)
        r2 = jnp.sum(s2, axis=1, keepdims=True)
        st_col[pl.ds(pl.multiple_of(base, B), B), :] = jnp.where(
            lanes == 0, r1, jnp.where(lanes == 1, r2, 0.0)
        )
        return carry

    lax.fori_loop(0, T // B, conv_tile, 0)
    st_s[...] = jnp.transpose(st_col[...])[0:8]
    st_sends = []
    for e in range(1, TP):
        cp = remote(
            st_s, st_r.at[e - 1], t_send.at[e - 1], t_recv.at[e - 1], (s, (t + e) % TP)
        )
        cp.start()
        st_sends.append(cp)

    relay(2, 1)

    scale2 = (HEAD_WIDTH + 64) ** (-0.5) * 1.4426950408889634
    mx[...] = jnp.full(mx.shape, -1e30, F32)
    acc[...] = jnp.zeros(acc.shape, F32)
    for k in (7, 8):
        w_copies[k].wait()
    QB = T // 2

    def attend(src):
        lat = kvb[src, :, 0:R, :].reshape(T, kvb.shape[3])
        k = dot(lat, v_kw[...]).astype(BF16)
        v = dot(lat, v_vw[...]).astype(BF16)
        ropes = []
        for r in range(CHUNKS):
            for g in range(4):
                tile = kvb[src, r, R:, 128 * g : 128 * (g + 1)].astype(F32)
                turned = pltpu.roll(tile, 64, 1)
                ropes.append(jnp.where(lane < 64, tile, turned).astype(BF16))
                ropes.append(jnp.where(lane < 64, turned, tile).astype(BF16))
        rope = jnp.concatenate(ropes, axis=0)
        ones = jnp.ones((T, 128), BF16)
        for h in range(H):
            hs = slice(128 * h, 128 * (h + 1))
            kc = jnp.concatenate([k[:, hs], rope], axis=1)
            vc = jnp.concatenate([v[:, hs], ones], axis=1)
            for qb in range(T // QB):
                rows = slice(qb * QB, (qb + 1) * QB)
                sc = dot_nt(qs[h, rows, :], kc)
                old = mx[h, rows, :]
                new = jnp.maximum(old, jnp.max(sc, axis=1, keepdims=True))
                mx[h, rows, :] = new
                alpha = jnp.exp2((old - new) * scale2)
                p = jnp.exp2((sc - new[:, 0:1]) * scale2).astype(BF16)
                acc[h, rows, :] = acc[h, rows, :] * jnp.concatenate([alpha, alpha], axis=1) + dot(p, vc)

    def key_step(d, carry):
        zd = jnp.where(z < Z // 2, lax.rem(z + d, Z), lax.rem(z - d + Z, Z))

        @pl.when(d > 0)
        def _():
            for i in range(CHUNKS // 2):
                arrived(zd * Y + y, (1 - c) + 2 * i)

        attend(zd * Y + y)

        @pl.when(d + 3 < Z)
        def _():
            relay(d + 3, 0)

        def across(e, carry2):
            src = zd * Y + lax.rem(y + e, Y)
            for i in range(CHUNKS // 2):
                arrived(src, c + 2 * i)
                mate_copy(src, i).start()
            for i in range(CHUNKS // 2):
                arrived(src, (1 - c) + 2 * i)
            attend(src)
            return carry2

        lax.fori_loop(1, Y, across, 0)

        @pl.when(d + 3 < Z)
        def _():
            relay(d + 3, 1)

        return carry

    sums = st_s[...]
    for e in range(1, TP):
        remote(
            st_s, st_r.at[e - 1], t_send.at[e - 1], t_recv.at[e - 1], (s, (t + e) % TP)
        ).wait_recv()
        sums += st_r[e - 1]
    cols = jnp.transpose(jnp.concatenate([sums] * 16, axis=0))
    mean = cols[:, 0:1] / (C * TP)
    square = cols[:, 1:2] / (C * TP)
    inv = lax.rsqrt(square - mean * mean + layer_eps)
    shaped = (conv[...] - mean) * inv * conv_gain[...]
    crs[...] = (shaped * jax.nn.sigmoid(shaped)).astype(BF16)

    lax.fori_loop(0, Z, key_step, 0)

    for h in range(H):
        ars[:, 128 * h : 128 * (h + 1)] = (acc[h, :, 0:128] / acc[h, :, 128:256]).astype(BF16)

    for k in (9, 10):
        w_copies[k].wait()
    NC = psb.shape[-1]
    NCH = D // NC

    def to_mate(n):
        return remote(psb.at[n, 1 - c], pr.at[n], p_send.at[n], p_recv.at[n], (s, mate))

    def across_chips(n, e):
        return remote(
            pa.at[n, e - 1], xr.at[n, e - 1], r_send.at[n, e - 1], r_recv.at[n, e - 1],
            (s, ((x + e) % X) * 2 + c),
        )

    def pair_sum(n):
        to_mate(n).wait_recv()
        for e in range(1, X):
            xd = (x + e) % X
            pa[n, e - 1] = (psb[n, c, xd].astype(F32) + pr[n, xd].astype(F32)).astype(BF16)
            across_chips(n, e).start()

    for n in range(NCH):
        cs = slice(n * NC, (n + 1) * NC)
        part = (dot(crs[...], v_cow[:, cs]) + dot(ars[...], v_aow[:, cs])).astype(BF16)
        for g in range(TP):
            psb[n, g % 2, g // 2] = part[g * Tb : (g + 1) * Tb]
        to_mate(n).start()
        if n > 0:
            pair_sum(n - 1)
    pair_sum(NCH - 1)

    merged = []
    square_sum = jnp.zeros((Tb, 1), F32)
    for n in range(NCH):
        m = psb[n, c, x].astype(F32) + pr[n, x].astype(F32)
        for e in range(1, X):
            across_chips(n, e).wait_recv()
            m += xr[n, e - 1].astype(F32)
        square_sum += jnp.sum(m * m, axis=1, keepdims=True)
        merged.append(m)
    inv_out = lax.rsqrt(square_sum / D + norm_eps)
    for n in range(NCH):
        cs = slice(n * NC, (n + 1) * NC)
        out[:, cs] = (merged[n] * inv_out * out_gain[:, cs]).astype(BF16)

    for cp in own_sends + fwd_sends + st_sends:
        cp.wait_send()

    @pl.when(s > 0)
    def _():
        halo(False).wait_send()

    @pl.when(s < S - 1)
    def _():
        halo(True).wait_send()

    def drain(zs, carry):
        for i in range(CHUNKS // 2):

            @pl.when((zs <= z) & (z + 1 < Z))
            def _():
                z_copy(zs, i, True).wait_send()

            @pl.when((zs >= z) & (z - 1 >= 0))
            def _():
                z_copy(zs, i, False).wait_send()

            for e in range(1, Y):
                y_copy(zs, i, e).wait_send()
                mate_copy(zs * Y + lax.rem(y + e, Y), i).wait_send()

            @pl.when(zs != z)
            def _():
                mate_copy(zs * Y + y, i).wait_send()

        return carry

    lax.fori_loop(0, Z, drain, 0)
    for n in range(NCH):
        to_mate(n).wait_send()
        for e in range(1, X):
            across_chips(n, e).wait_send()


def local(S, TP, *args):
    (tokens, in_gain, cvw, cgw, taps, conv_gain, qlw, lw, rkw, q_gain, l_gain,
     qw, qrw, kw, vw, cow, aow, out_gain) = args
    T, F = tokens.shape
    D = F * TP
    C = cvw.shape[1]
    H = kw.shape[1] // HEAD_WIDTH
    QL, L = qlw.shape[1], lw.shape[1]
    RW = rkw.shape[1]
    Y = 1
    while 2 * (2 * Y) ** 2 <= S:
        Y *= 2
    Z, X = S // Y, TP // 2
    cfg = (S, TP, Z, Y, X, T, F, D, C, H)
    R = T // CHUNKS
    Tb = T // TP
    NC = D // 4

    positions = (lax.axis_index("sp") * T + jnp.arange(T, dtype=jnp.int32)).astype(F32)
    half = RW // 2
    inverse = rope_base ** (-jnp.arange(half, dtype=F32) / half)
    angles = positions[:, None] * inverse[None, :]
    co, si = jnp.cos(angles), jnp.sin(angles)
    cosine = jnp.concatenate([co] * 4, axis=1)
    sine = jnp.concatenate([-si, si] * 2, axis=1)
    rkw2 = jnp.concatenate([rkw, rkw], axis=1)
    q3 = qrw.reshape(QL, H, RW)
    qrw2 = jnp.concatenate([q3, q3], axis=2).reshape(QL, H * 2 * RW)

    row = lambda v: v.reshape(1, -1)
    hbm = pl.BlockSpec(memory_space=pl.ANY)
    vm = pl.BlockSpec(memory_space=pltpu.VMEM)
    V = pltpu.VMEM
    sem = pltpu.SemaphoreType.DMA
    return pl.pallas_call(
        functools.partial(layer, cfg),
        out_shape=jax.ShapeDtypeStruct((Tb, D), BF16),
        in_specs=[hbm, vm, hbm, hbm, vm, vm, hbm, hbm, hbm, vm, vm,
                  hbm, hbm, hbm, hbm, hbm, hbm, vm, vm, vm],
        out_specs=vm,
        scratch_shapes=[
            V((TP, T, F), BF16),
            V((D, C), BF16), V((D, C), BF16), V((D, QL), BF16), V((D, L), BF16),
            V((D, 2 * RW), BF16), V((QL, H * 128), BF16), V((QL, H * 128), BF16),
            V((L, H * 128), BF16), V((L, H * 128), BF16), V((C, D), BF16), V((H * 128, D), BF16),
            V((T, D), BF16),
            V((S, CHUNKS, R + R // 8, L), BF16),
            V((2, 16, C), BF16), V((2, 16, C), BF16),
            V((C // 128, T + 32, 128), F32), V((T, C), F32),
            V((T, 128), F32), V((8, T), F32), V((TP - 1, 8, T), F32),
            V((T, C), BF16),
            V((H, T, 256), BF16), V((H, T, 128), F32), V((H, T, 256), F32),
            V((T, H * 128), BF16),
            V((4, 2, X, Tb, NC), BF16), V((4, X, Tb, NC), BF16),
            V((4, X - 1, Tb, NC), BF16), V((4, X - 1, Tb, NC), BF16),
            sem((CHUNKS,)), sem((11,)), sem((X, CHUNKS)), sem((X - 1, CHUNKS)), sem((TP, CHUNKS)),
            sem((S, CHUNKS)), sem((2, Z, CHUNKS // 2)), sem((Y - 1, Z, CHUNKS // 2)),
            sem((S, CHUNKS // 2)),
            sem((2,)), sem((2,)), sem((TP - 1,)), sem((TP - 1,)),
            sem((4,)), sem((4,)), sem((4, X - 1)), sem((4, X - 1)),
        ],
        compiler_params=pltpu.CompilerParams(
            collective_id=0, has_side_effects=True, vmem_limit_bytes=67043328
        ),
    )(
        tokens, row(in_gain), cvw, cgw, taps, row(conv_gain), qlw, lw, rkw2, row(q_gain),
        row(l_gain), qw, qrw2, kw, vw, cow, aow, row(out_gain), cosine, sine,
    )


def solution(mesh):
    sizes = mesh.shape
    return jax.shard_map(
        functools.partial(local, sizes["sp"], sizes["tp"]),
        mesh=mesh,
        in_specs=(
            P("sp", "tp"), P(), P(None, "tp"), P(None, "tp"), P(None, "tp"), P("tp"),
            P(), P(), P(), P(), P(),
            P(None, "tp"), P(None, "tp"), P(None, "tp"), P(None, "tp"),
            P("tp", None), P("tp", None), P(),
        ),
        out_specs=P(("sp", "tp"), None),
        check_vma=False,
    )
```
